32 devices in a mesh: sp: 4 (over y, x), dp: 8 (over z, core).
Axes of the slice: x: 2, y: 2, z: 4, core: 2. Of those that a mesh axis runs over, the one named last changes fastest.
Arguments:
- tokens: bfloat16 [8, 1280, 2048], P('dp', 'sp'), may hold values from -6 to 6
- up_weight: bfloat16 [2048, 2048], P('dp'), may hold values from -0.125 to 0.125
- gate_weight: bfloat16 [2048, 2048], P('dp'), may hold values from -0.125 to 0.125
- group_gain: float32 [16, 128], P('sp'), may hold values from 0.1 to 1.9
- mix_weight: bfloat16 [16, 1280, 1280], P('sp', 'dp'), may hold values from -0.15625 to 0.15625
- mix_bias: float32 [16, 1280], P('sp'), may hold values from 0.5 to 1.5
- out_gain: float32 [2048], replicated, may hold values from 0.1 to 1.9
- out_weight: bfloat16 [2048, 2048], P(None, 'dp'), may hold values from -0.125 to 0.125
Outputs:
- mixed_out: bfloat16 [8, 1280, 2048], P('dp', 'sp')
The draws below stay inside these ranges and needn't reach their ends.
All inputs are finite; a program needn't handle non-finite values.
Results may differ from the reference program's by a relative error of at most 0.0072.
Values may be sent and summed in bfloat16 or wider, within the bound.
A program may use at most 128 MiB of HBM per device.

```python
import jax
import jax.numpy as jnp
from jax import lax

D = 2048
GROUPS = 16
GROUP_DIM = 128
SPAN = 1280
WIDTH = 2048
LENGTH = 1280
SEQS = 8


def level_of(key, extent, cuts, smallest, top_value):
    level, own = 1.0, jax.random.fold_in(key, 6)
    for axis_at, parts in cuts:
        steps = jnp.exp(jax.random.uniform(jax.random.fold_in(own, axis_at), (parts,), jnp.float32, smallest / len(cuts), top_value / len(cuts)))
        level = level * jnp.repeat(steps, extent[axis_at] // parts).reshape([-1 if axis == axis_at else 1 for axis in range(len(extent))])
    return level


def normal_values(own_key, dims, deviation, most, cuts=(), held_as=jnp.bfloat16):
    entries = deviation * jax.random.normal(own_key, dims, jnp.float32)
    if cuts:
        entries = entries * level_of(own_key, dims, cuts, -0.22, 0.18)
    return jnp.clip(entries, -most, most).astype(held_as)


def setup_inputs(seed: int = 0) -> dict:
    splits = jax.random.split(jax.random.key(seed), 9)
    tokens = normal_values(splits[0], (SEQS, LENGTH, D), 1.0, 6.0, ((0, 8), (1, 4)))
    up_weight = normal_values(splits[1], (D, WIDTH), D ** -0.5, 0.125, ((0, 8),))
    gate_weight = normal_values(splits[2], (D, WIDTH), D ** -0.5, 0.125, ((0, 8),))
    group_gain = jnp.clip(1.0 + 0.18 * jax.random.normal(splits[3], (GROUPS, GROUP_DIM), jnp.float32), 0.1, 1.9)
    mix_weight = normal_values(splits[4], (GROUPS, SPAN, SPAN), SPAN ** -0.5, 0.15625, ((0, 4), (1, 8)))
    mix_bias = jnp.clip(0.5 + 1.0 * jax.random.uniform(splits[5], (GROUPS, SPAN), jnp.float32) ** level_of(splits[5], (GROUPS, SPAN), ((0, 4),), -0.2, 0.2), 0.5, 1.5)
    out_gain = jnp.clip(1.0 + 0.18 * jax.random.normal(splits[6], (WIDTH,), jnp.float32), 0.1, 1.9)
    out_weight = normal_values(splits[7], (WIDTH, D), WIDTH ** -0.5, 0.125, ((1, 8),))
    return {"tokens": tokens, "up_weight": up_weight, "gate_weight": gate_weight, "group_gain": group_gain, "mix_weight": mix_weight, "mix_bias": mix_bias, "out_gain": out_gain, "out_weight": out_weight}


norm_eps = 1e-06

def reference(tokens, up_weight, gate_weight, group_gain, mix_weight, mix_bias, out_gain, out_weight):
    lower = jnp.tril(jnp.ones((SPAN, SPAN), dtype=bool))
    mix_mask = jnp.where(lower[None], mix_weight, jnp.zeros_like(mix_weight)).astype(jnp.float32)
    bias_cols = mix_bias.astype(jnp.float32).T

    def one_sequence(sequence):
        up_proj = jnp.dot(sequence, up_weight, preferred_element_type=jnp.float32).astype(jnp.bfloat16)
        gate_proj = jnp.dot(sequence, gate_weight, preferred_element_type=jnp.float32).astype(jnp.bfloat16)
        up_proj = lax.optimization_barrier(up_proj)
        gate_proj = lax.optimization_barrier(gate_proj)
        opened = jax.nn.gelu(up_proj.astype(jnp.float32)).reshape(LENGTH, GROUPS, GROUP_DIM)
        gate_act = jax.nn.gelu(gate_proj.astype(jnp.float32)).reshape(LENGTH, GROUPS, GROUP_DIM)
        center = lax.optimization_barrier(jnp.mean(gate_act, axis=-1, keepdims=True))
        spread = lax.optimization_barrier(jnp.mean(jnp.square(gate_act - center), axis=-1, keepdims=True))
        normal_v = ((gate_act - center) * lax.rsqrt(spread + norm_eps) * group_gain.astype(jnp.float32)).astype(jnp.bfloat16)
        normal_v = lax.optimization_barrier(normal_v)
        blocks = normal_v.astype(jnp.float32).reshape(LENGTH // SPAN, SPAN, GROUPS, GROUP_DIM)
        mixed_sum = jnp.einsum('gij,njgc->nigc', mix_mask, blocks) + bias_cols[None, :, :, None]
        gated = (opened * mixed_sum.reshape(LENGTH, GROUPS, GROUP_DIM)).astype(jnp.bfloat16)
        gated = lax.optimization_barrier(gated)
        gated_f = gated.astype(jnp.float32).reshape(LENGTH, WIDTH)
        scale = lax.rsqrt(lax.optimization_barrier(jnp.mean(gated_f * gated_f, axis=-1, keepdims=True)) + norm_eps)
        normed = (gated_f * scale * out_gain.astype(jnp.float32)).astype(jnp.bfloat16)
        return jnp.dot(normed, out_weight, preferred_element_type=jnp.float32).astype(jnp.bfloat16)
    return lax.map(one_sequence, tokens)
```

```python
import functools

import jax
import jax.numpy as jnp
from jax import lax
from jax.experimental import pallas as pl
from jax.experimental.pallas import tpu as pltpu
from jax.sharding import PartitionSpec as P

norm_eps = 1e-06
CORES = 2
MESH = pl.DeviceIdType.MESH


def gather_kernel(sp, zs, tok_ref, up_ref, gate_ref, mix_ref, outw_ref,
                  tok_full, ug_full, mix_full, out_full,
                  tok_v, ug_v, mix_v, outw_v,
                  load_sem, loc_sem, line_recv, up_send, down_send, part_send, part_recv,
                  tok_send, tok_recv, plane_send, plane_recv, pp_send, pp_recv):
    me = lax.axis_index("sp")
    dp = lax.axis_index("dp")
    z, c = dp // CORES, lax.rem(dp, CORES)
    groups, rows, block = mix_v.shape
    chans, ncol = outw_v.shape
    items = 2 + groups
    cut = pl.ds(pl.multiple_of(me * chans, 128), chans)

    loads = [
        pltpu.make_async_copy(tok_ref, tok_v, load_sem.at[0]),
        pltpu.make_async_copy(outw_ref.at[cut, :], outw_v, load_sem.at[1]),
        pltpu.make_async_copy(up_ref.at[:, cut], ug_v.at[0], load_sem.at[2]),
        pltpu.make_async_copy(gate_ref.at[:, cut], ug_v.at[1], load_sem.at[3]),
        pltpu.make_async_copy(mix_ref, mix_v, load_sem.at[4]),
    ]
    for load in loads:
        load.start()

    def at_line(zz):
        return {"dp": zz * CORES + c}

    partner = {"dp": z * CORES + (1 - c)}

    def peer(r):
        return {"sp": lax.rem(me + r, sp)}

    def width(o):
        return min(block, -(-((o + 1) * CORES * rows) // 128) * 128)

    def place(i, o, cc):
        if i == 0:
            return out_full.at[cc, me, :, pl.ds(o * ncol, ncol)]
        if i == 1:
            return ug_full.at[:, o * CORES + cc]
        return mix_full.at[i - 2, o * CORES + cc, :, pl.ds(0, width(o))]

    def own(i, zz):
        if i == 0:
            return outw_v
        if i == 1:
            return ug_v
        return mix_v.at[i - 2, :, pl.ds(0, width(zz))]

    def remote(src, dst, send, recv, device):
        return pltpu.make_async_remote_copy(
            src_ref=src, dst_ref=dst, send_sem=send, recv_sem=recv,
            device_id=device, device_id_type=MESH)

    def run(zz):
        sends, locs = [], []
        barrier = pltpu.get_barrier_semaphore()
        friends = [partner] + [peer(r) for r in range(1, sp)]
        if zz > 0:
            friends.append(at_line(zz - 1))
        if zz < zs - 1:
            friends.append(at_line(zz + 1))
        for friend in friends:
            pl.semaphore_signal(barrier, inc=1, device_id=friend, device_id_type=MESH)
        pl.semaphore_wait(barrier, len(friends))

        def push(copy):
            copy.start()
            sends.append(copy)

        def spread(i, o, src):
            dst = place(i, o, c)
            if o >= zz and zz > 0:
                push(remote(src, dst, down_send.at[i, o], line_recv.at[i, o], at_line(zz - 1)))
            if o <= zz and zz < zs - 1:
                push(remote(src, dst, up_send.at[i, o], line_recv.at[i, o], at_line(zz + 1)))
            push(remote(src, dst, part_send.at[i, o], part_recv.at[i, o], partner))

        def start_own(i):
            if i == 0:
                loads[1].wait()
            elif i == 1:
                loads[2].wait()
                loads[3].wait()
            elif i == 2:
                loads[4].wait()
            src = own(i, zz)
            spread(i, zz, src)
            copy = pltpu.make_async_copy(src, place(i, zz, c), loc_sem.at[i])
            copy.start()
            locs.append(copy)

        start_own(0)
        loads[0].wait()
        for r in range(1, sp):
            push(remote(tok_v, tok_full.at[me], tok_send.at[r], tok_recv.at[r], peer(r)))
        tok_copy = pltpu.make_async_copy(tok_v, tok_full.at[me], loc_sem.at[items])
        tok_copy.start()
        for i in range(items):
            if i + 1 < items:
                start_own(i + 1)
            for k in range(1, zs):
                for o in (zz + k, zz - k):
                    if 0 <= o < zs:
                        spot = place(i, o, c)
                        remote(spot, spot, up_send.at[i, o], line_recv.at[i, o], partner).wait_recv()
                        spread(i, o, spot)
            if i == 0:
                locs[0].wait()
                spot = out_full.at[c, me]
                for r in range(1, sp):
                    push(remote(spot, spot, plane_send.at[r], plane_recv.at[r], peer(r)))
        for r in range(1, sp):
            spot = out_full.at[c, lax.rem(me + sp - r, sp)]
            remote(spot, spot, plane_send.at[r], plane_recv.at[r], partner).wait_recv()
            push(remote(spot, spot, pp_send.at[r], pp_recv.at[r], partner))
        for i in range(items):
            for o in range(zs):
                spot = place(i, o, 1 - c)
                remote(spot, spot, part_send.at[i, o], part_recv.at[i, o], partner).wait_recv()
        for r in range(1, sp):
            source = lax.rem(me + sp - r, sp)
            spot = out_full.at[1 - c, source]
            remote(spot, spot, pp_send.at[r], pp_recv.at[r], partner).wait_recv()
            spot = tok_full.at[source]
            remote(spot, spot, tok_send.at[r], tok_recv.at[r], partner).wait_recv()
        for copy in sends:
            copy.wait_send()
        tok_copy.wait()
        for copy in locs[1:]:
            copy.wait()

    for zz in range(zs):
        pl.when(z == zz)(functools.partial(run, zz))


def gather_all(tokens, up_weight, gate_weight, mix_weight, out_weight, chans):
    sp, dps = lax.axis_size("sp"), lax.axis_size("dp")
    zs = dps // CORES
    groups, rows, block = mix_weight.shape
    depth = up_weight.shape[0]
    ncol = out_weight.shape[1]
    items = 2 + groups
    bf = jnp.bfloat16
    dma = pltpu.SemaphoreType.DMA
    return pl.pallas_call(
        functools.partial(gather_kernel, sp, zs),
        out_shape=(
            jax.ShapeDtypeStruct((sp,) + tokens.shape, bf),
            jax.ShapeDtypeStruct((2, dps, depth, chans), bf),
            jax.ShapeDtypeStruct((groups, dps, rows, block), bf),
            jax.ShapeDtypeStruct((CORES, sp, chans, zs * ncol), bf),
        ),
        in_specs=[pl.BlockSpec(memory_space=pl.ANY)] * 5,
        out_specs=[pl.BlockSpec(memory_space=pl.ANY)] * 4,
        scratch_shapes=[
            pltpu.VMEM(tokens.shape, bf),
            pltpu.VMEM((2, depth, chans), bf),
            pltpu.VMEM(mix_weight.shape, bf),
            pltpu.VMEM((chans, ncol), bf),
            dma((5,)),
            dma((items + 1,)),
            dma((items, zs)),
            dma((items, zs)),
            dma((items, zs)),
            dma((items, zs)),
            dma((items, zs)),
        ] + [dma((sp,))] * 6,
        compiler_params=pltpu.CompilerParams(collective_id=0, has_side_effects=True),
    )(tokens, up_weight, gate_weight, mix_weight, out_weight)


def body(tokens, up_weight, gate_weight, group_gain, mix_weight, mix_bias, out_gain, out_weight):
    sequences, per_device, model_width = tokens.shape
    groups_dev, group_dim = group_gain.shape
    sp = lax.axis_size("sp")
    chans = groups_dev * group_dim
    seq_len = per_device * sp
    tok_full, ug_full, mix_full, out_full = gather_all(
        tokens, up_weight, gate_weight, mix_weight, out_weight, chans
    )
    flat = jnp.moveaxis(tok_full, 0, 1).reshape(sequences * seq_len, model_width)
    ug = ug_full.reshape(2, model_width, chans)
    block_len = mix_full.shape[3]
    full_mix = mix_full.reshape(groups_dev, block_len, block_len)
    up_proj = jnp.dot(flat, ug[0], preferred_element_type=jnp.float32).astype(jnp.bfloat16)
    gate_proj = jnp.dot(flat, ug[1], preferred_element_type=jnp.float32).astype(jnp.bfloat16)
    up_heads = up_proj.reshape(sequences, seq_len, groups_dev, group_dim)
    gate_heads = gate_proj.reshape(sequences, seq_len, groups_dev, group_dim)
    opened = jax.nn.gelu(up_heads.astype(jnp.float32))
    gate_act = jax.nn.gelu(gate_heads.astype(jnp.float32))
    center = jnp.mean(gate_act, axis=-1, keepdims=True)
    spread = jnp.mean(jnp.square(gate_act - center), axis=-1, keepdims=True)
    normal_v = ((gate_act - center) * lax.rsqrt(spread + norm_eps) * group_gain).astype(
        jnp.bfloat16
    )
    lower = jnp.tril(jnp.ones((block_len, block_len), dtype=bool))
    masked_mix = jnp.where(lower[None], full_mix, jnp.zeros_like(full_mix))
    blocks = normal_v.reshape(sequences, seq_len // block_len, block_len, groups_dev, group_dim)
    mixed_sum = jnp.einsum(
        "gij,snjgc->snigc", masked_mix, blocks, preferred_element_type=jnp.float32
    )
    mixed_sum = mixed_sum + mix_bias.T[None, None, :, :, None]
    gated = (opened * mixed_sum.reshape(sequences, seq_len, groups_dev, group_dim)).astype(
        jnp.bfloat16
    ).reshape(sequences, seq_len, chans)
    by_token = lax.all_to_all(gated, "sp", split_axis=1, concat_axis=2, tiled=True)
    gated_f = by_token.reshape(sequences * per_device, sp * chans).astype(jnp.float32)
    scale = lax.rsqrt(jnp.mean(gated_f * gated_f, axis=-1, keepdims=True) + norm_eps)
    normed = (gated_f * scale * out_gain).astype(jnp.bfloat16)
    halves = out_full.reshape(CORES, sp * chans, -1)
    ncol = out_weight.shape[1]
    parts = [
        jnp.dot(normed, halves[h], preferred_element_type=jnp.float32)
        .astype(jnp.bfloat16)
        .reshape(sequences, per_device, -1, 1, ncol)
        for h in range(CORES)
    ]
    return jnp.concatenate(parts, axis=3).reshape(sequences, per_device, model_width)


def solution(mesh):
    return jax.shard_map(
        body,
        mesh=mesh,
        in_specs=(
            P("dp", "sp", None),
            P("dp", None),
            P("dp", None),
            P("sp", None),
            P("sp", "dp", None),
            P("sp", None),
            P(),
            P(None, "dp"),
        ),
        out_specs=P("dp", "sp", None),
        check_vma=False,
    )
```

```python
import functools

import jax
import jax.numpy as jnp
from jax import lax
from jax.experimental import pallas as pl
from jax.experimental.pallas import tpu as pltpu
from jax.sharding import PartitionSpec as P

norm_eps = 1e-06
CORES = 2
MESH = pl.DeviceIdType.MESH


def gather_kernel(sp, zs, tok_ref, up_ref, gate_ref, mix_ref, outw_ref,
                  tok_full, ug_full, mix_full, out_full,
                  tok_v, ug_v, mix_v, outw_v,
                  load_sem, loc_sem, line_recv, up_send, down_send, part_send, part_recv,
                  tok_send, tok_recv, plane_send, plane_recv, pp_send, pp_recv):
    me = lax.axis_index("sp")
    dp = lax.axis_index("dp")
    z, c = dp // CORES, lax.rem(dp, CORES)
    groups, rows, block = mix_v.shape
    chans, ncol = outw_v.shape
    items = 2 + groups
    cut = pl.ds(pl.multiple_of(me * chans, 128), chans)

    loads = [
        pltpu.make_async_copy(tok_ref, tok_v, load_sem.at[0]),
        pltpu.make_async_copy(outw_ref.at[cut, :], outw_v, load_sem.at[1]),
        pltpu.make_async_copy(up_ref.at[:, cut], ug_v.at[0], load_sem.at[2]),
        pltpu.make_async_copy(gate_ref.at[:, cut], ug_v.at[1], load_sem.at[3]),
        pltpu.make_async_copy(mix_ref, mix_v, load_sem.at[4]),
    ]
    for load in loads:
        load.start()

    def at_line(zz):
        return {"dp": zz * CORES + c}

    partner = {"dp": z * CORES + (1 - c)}

    def peer(r):
        return {"sp": lax.rem(me + r, sp)}

    def width(o):
        return min(block, -(-((o + 1) * CORES * rows) // 128) * 128)

    def place(i, o, cc):
        if i == 0:
            return out_full.at[cc, me, :, pl.ds(o * ncol, ncol)]
        if i == 1:
            return ug_full.at[:, o * CORES + cc]
        return mix_full.at[i - 2, o * CORES + cc, :, pl.ds(0, width(o))]

    def own(i, zz):
        if i == 0:
            return outw_v
        if i == 1:
            return ug_v
        return mix_v.at[i - 2, :, pl.ds(0, width(zz))]

    def remote(src, dst, send, recv, device):
        return pltpu.make_async_remote_copy(
            src_ref=src, dst_ref=dst, send_sem=send, recv_sem=recv,
            device_id=device, device_id_type=MESH)

    def run(zz):
        sends, locs = [], []
        barrier = pltpu.get_barrier_semaphore()
        friends = [partner] + [peer(r) for r in range(1, sp)]
        if zz > 0:
            friends.append(at_line(zz - 1))
        if zz < zs - 1:
            friends.append(at_line(zz + 1))
        for friend in friends:
            pl.semaphore_signal(barrier, inc=1, device_id=friend, device_id_type=MESH)
        pl.semaphore_wait(barrier, len(friends))

        def push(copy):
            copy.start()
            sends.append(copy)

        def spread(i, o, src):
            dst = place(i, o, c)
            if o >= zz and zz > 0:
                push(remote(src, dst, down_send.at[i, o], line_recv.at[i, o], at_line(zz - 1)))
            if o <= zz and zz < zs - 1:
                push(remote(src, dst, up_send.at[i, o], line_recv.at[i, o], at_line(zz + 1)))
            push(remote(src, dst, part_send.at[i, o], part_recv.at[i, o], partner))

        def start_own(i):
            if i == 0:
                loads[1].wait()
            elif i == 1:
                loads[2].wait()
                loads[3].wait()
            elif i == 2:
                loads[4].wait()
            src = own(i, zz)
            spread(i, zz, src)
            copy = pltpu.make_async_copy(src, place(i, zz, c), loc_sem.at[i])
            copy.start()
            locs.append(copy)

        start_own(0)
        loads[0].wait()
        for r in range(1, sp):
            push(remote(tok_v, tok_full.at[me], tok_send.at[r], tok_recv.at[r], peer(r)))
        tok_copy = pltpu.make_async_copy(tok_v, tok_full.at[me], loc_sem.at[items])
        tok_copy.start()
        for i in range(items):
            if i + 1 < items:
                start_own(i + 1)
            for k in range(1, zs):
                for o in (zz + k, zz - k):
                    if 0 <= o < zs:
                        spot = place(i, o, c)
                        remote(spot, spot, up_send.at[i, o], line_recv.at[i, o], partner).wait_recv()
                        spread(i, o, spot)
            if i == 0:
                locs[0].wait()
                spot = out_full.at[c, me]
                for r in range(1, sp):
                    push(remote(spot, spot, plane_send.at[r], plane_recv.at[r], peer(r)))
        for r in range(1, sp):
            spot = out_full.at[c, lax.rem(me + sp - r, sp)]
            remote(spot, spot, plane_send.at[r], plane_recv.at[r], partner).wait_recv()
            push(remote(spot, spot, pp_send.at[r], pp_recv.at[r], partner))
        for i in range(items):
            for o in range(zs):
                spot = place(i, o, 1 - c)
                remote(spot, spot, part_send.at[i, o], part_recv.at[i, o], partner).wait_recv()
        for r in range(1, sp):
            source = lax.rem(me + sp - r, sp)
            spot = out_full.at[1 - c, source]
            remote(spot, spot, pp_send.at[r], pp_recv.at[r], partner).wait_recv()
            spot = tok_full.at[source]
            remote(spot, spot, tok_send.at[r], tok_recv.at[r], partner).wait_recv()
        for copy in sends:
            copy.wait_send()
        tok_copy.wait()
        for copy in locs[1:]:
            copy.wait()

    for zz in range(zs):
        pl.when(z == zz)(functools.partial(run, zz))


def gather_all(tokens, up_weight, gate_weight, mix_weight, out_weight, chans):
    sp, dps = lax.axis_size("sp"), lax.axis_size("dp")
    zs = dps // CORES
    groups, rows, block = mix_weight.shape
    depth = up_weight.shape[0]
    ncol = out_weight.shape[1]
    items = 2 + groups
    bf = jnp.bfloat16
    dma = pltpu.SemaphoreType.DMA
    return pl.pallas_call(
        functools.partial(gather_kernel, sp, zs),
        out_shape=(
            jax.ShapeDtypeStruct((sp,) + tokens.shape, bf),
            jax.ShapeDtypeStruct((2, dps, depth, chans), bf),
            jax.ShapeDtypeStruct((groups, dps, rows, block), bf),
            jax.ShapeDtypeStruct((CORES, sp, chans, zs * ncol), bf),
        ),
        in_specs=[pl.BlockSpec(memory_space=pl.ANY)] * 5,
        out_specs=[pl.BlockSpec(memory_space=pl.ANY)] * 4,
        scratch_shapes=[
            pltpu.VMEM(tokens.shape, bf),
            pltpu.VMEM((2, depth, chans), bf),
            pltpu.VMEM(mix_weight.shape, bf),
            pltpu.VMEM((chans, ncol), bf),
            dma((5,)),
            dma((items + 1,)),
            dma((items, zs)),
            dma((items, zs)),
            dma((items, zs)),
            dma((items, zs)),
            dma((items, zs)),
        ] + [dma((sp,))] * 6,
        compiler_params=pltpu.CompilerParams(collective_id=0, has_side_effects=True),
    )(tokens, up_weight, gate_weight, mix_weight, out_weight)


def mixer_kernel(flat_ref, ug_ref, gain_ref, mix_ref, bias_ref, out_ref, w_v, open_v, norm_v):
    block, dim = out_ref.shape
    step = 256 if block % 256 == 0 else block
    w_v[:, :dim] = ug_ref[0]
    w_v[:, dim:] = ug_ref[1]

    @pl.loop(0, block // step)
    def _(b):
        rows = pl.ds(pl.multiple_of(b * step, step), step)
        both = jnp.dot(flat_ref[rows, :], w_v[...], preferred_element_type=jnp.float32)
        both = jax.nn.gelu(both.astype(jnp.bfloat16).astype(jnp.float32))
        open_v[rows, :] = both[:, :dim]
        act = both[:, dim:]
        act = act - jnp.mean(act, axis=-1, keepdims=True)
        spread = jnp.mean(act * act, axis=-1, keepdims=True)
        norm_v[rows, :] = (act * lax.rsqrt(spread + norm_eps) * gain_ref[0]).astype(jnp.bfloat16)

    keep = lax.broadcasted_iota(jnp.int32, (step, step), 0) >= lax.broadcasted_iota(
        jnp.int32, (step, step), 1
    )
    for b in range(block // step):
        lo, hi = b * step, (b + 1) * step
        corner = jnp.where(keep, mix_ref[0, lo:hi, lo:hi].astype(jnp.float32), 0.0)
        total = jnp.dot(
            corner.astype(jnp.bfloat16), norm_v[lo:hi, :], preferred_element_type=jnp.float32
        )
        if b > 0:
            total += jnp.dot(
                mix_ref[0, lo:hi, :lo], norm_v[:lo, :], preferred_element_type=jnp.float32
            )
        total += jnp.broadcast_to(bias_ref[0, :, lo:hi], (dim, step)).T
        out_ref[lo:hi, :] = (open_v[lo:hi, :] * total).astype(jnp.bfloat16)


def mixer(flat, ug, group_gain, full_mix, mix_bias):
    groups, block, _ = full_mix.shape
    dim = group_gain.shape[1]
    total, width = flat.shape
    return pl.pallas_call(
        mixer_kernel,
        grid=(total // block, groups),
        out_shape=jax.ShapeDtypeStruct((total, groups * dim), jnp.bfloat16),
        in_specs=[
            pl.BlockSpec((block, width), lambda n, g: (n, 0)),
            pl.BlockSpec((2, width, dim), lambda n, g: (0, 0, g)),
            pl.BlockSpec((1, 1, dim), lambda n, g: (g, 0, 0)),
            pl.BlockSpec((1, block, block), lambda n, g: (g, 0, 0)),
            pl.BlockSpec((1, 1, block), lambda n, g: (g, 0, 0)),
        ],
        out_specs=pl.BlockSpec((block, dim), lambda n, g: (n, g)),
        scratch_shapes=[
            pltpu.VMEM((width, 2 * dim), jnp.bfloat16),
            pltpu.VMEM((block, dim), jnp.float32),
            pltpu.VMEM((block, dim), jnp.bfloat16),
        ],
    )(flat, ug, group_gain[:, None, :], full_mix, mix_bias[:, None, :])


def finish_kernel(sp, gated_ref, gain_ref, w_ref, out_ref, held, normed, send_sem, recv_sem):
    me = lax.axis_index("sp")
    rows, chans = held.shape[1:]
    ncol = out_ref.shape[2]
    barrier = pltpu.get_barrier_semaphore()
    for r in range(1, sp):
        pl.semaphore_signal(
            barrier, inc=1, device_id={"sp": lax.rem(me + r, sp)}, device_id_type=MESH
        )
    pl.semaphore_wait(barrier, sp - 1)
    copies = []
    for r in range(1, sp):
        to = lax.rem(me + r, sp)
        copies.append(
            pltpu.make_async_remote_copy(
                src_ref=gated_ref.at[to], dst_ref=held.at[me],
                send_sem=send_sem.at[r], recv_sem=recv_sem.at[r],
                device_id={"sp": to}, device_id_type=MESH)
        )
    for copy in copies:
        copy.start()
    held[me] = gated_ref[me]
    for copy in copies:
        copy.wait()
    squares = jnp.zeros((rows, 1), jnp.float32)
    for s in range(sp):
        part = held[s].astype(jnp.float32)
        squares += jnp.sum(part * part, axis=-1, keepdims=True)
    scale = lax.rsqrt(squares / (sp * chans) + norm_eps)
    for s in range(sp):
        cols = slice(s * chans, (s + 1) * chans)
        normed[:, cols] = (held[s].astype(jnp.float32) * scale * gain_ref[:, cols]).astype(
            jnp.bfloat16
        )

    @pl.loop(0, w_ref.shape[2] // ncol)
    def _(o):
        for h in range(CORES):
            cols = pl.ds(pl.multiple_of(o * ncol, ncol), ncol)
            out_ref[o * CORES + h] = jnp.dot(
                normed[...], w_ref[h, :, cols], preferred_element_type=jnp.float32
            ).astype(jnp.bfloat16)


def finish(gated, out_gain, halves, ncol):
    sp, rows, chans = gated.shape
    vmem = pl.BlockSpec(memory_space=pltpu.VMEM)
    return pl.pallas_call(
        functools.partial(finish_kernel, sp),
        out_shape=jax.ShapeDtypeStruct((CORES * halves.shape[2] // ncol, rows, ncol), jnp.bfloat16),
        in_specs=[vmem] * 3,
        out_specs=vmem,
        scratch_shapes=[
            pltpu.VMEM(gated.shape, jnp.bfloat16),
            pltpu.VMEM((rows, sp * chans), jnp.bfloat16),
            pltpu.SemaphoreType.DMA((sp,)),
            pltpu.SemaphoreType.DMA((sp,)),
        ],
        compiler_params=pltpu.CompilerParams(collective_id=1, has_side_effects=True),
    )(gated, out_gain[None, :], halves)


def body(tokens, up_weight, gate_weight, group_gain, mix_weight, mix_bias, out_gain, out_weight):
    sequences, per_device, model_width = tokens.shape
    groups_dev, group_dim = group_gain.shape
    sp = lax.axis_size("sp")
    chans = groups_dev * group_dim
    seq_len = per_device * sp
    tok_full, ug_full, mix_full, out_full = gather_all(
        tokens, up_weight, gate_weight, mix_weight, out_weight, chans
    )
    flat = jnp.moveaxis(tok_full, 0, 1).reshape(sequences * seq_len, model_width)
    ug = ug_full.reshape(2, model_width, chans)
    block_len = mix_full.shape[3]
    full_mix = mix_full.reshape(groups_dev, block_len, block_len)
    gated = mixer(flat, ug, group_gain, full_mix, mix_bias)
    gated = jnp.moveaxis(gated.reshape(sequences, sp, per_device, chans), 1, 0)
    gated = gated.reshape(sp, sequences * per_device, chans)
    halves = out_full.reshape(CORES, sp * chans, -1)
    output = finish(gated, out_gain, halves, out_weight.shape[1])
    return jnp.moveaxis(output, 0, 1).reshape(sequences, per_device, model_width)


def solution(mesh):
    return jax.shard_map(
        body,
        mesh=mesh,
        in_specs=(
            P("dp", "sp", None),
            P("dp", None),
            P("dp", None),
            P("sp", None),
            P("sp", "dp", None),
            P("sp", None),
            P(),
            P(None, "dp"),
        ),
        out_specs=P("dp", "sp", None),
        check_vma=False,
    )
```
